32 devices in a mesh: sp: 8 (over z, y), tp: 4 (over x, core).
Axes of the slice: x: 2, y: 2, z: 4, core: 2. Of those that a mesh axis runs over, the one named last changes fastest.
Arguments:
- resid: bfloat16 [1536, 2048], P('sp'), may hold values from -6 to 6
- query_broad: bfloat16 [1536, 1536], P('sp', 'tp'), may hold values from -60 to 60
- query_narrow: bfloat16 [1536, 1024], P('sp', 'tp'), may hold values from -60 to 60
- latent: bfloat16 [1536, 512], P('sp'), may hold values from -6 to 6
- key_rope: bfloat16 [1536, 64], P('sp'), may hold values from -6 to 6
- latent_gain: float32 [512], replicated, may hold values from 0.1 to 1.9
- key_up_broad: bfloat16 [512, 1024], P(None, 'tp'), may hold values from -0.25 to 0.25
- value_up_broad: bfloat16 [512, 1024], P(None, 'tp'), may hold values from -0.25 to 0.25
- key_up_narrow: bfloat16 [512, 512], P(None, 'tp'), may hold values from -0.25 to 0.25
- value_up_narrow: bfloat16 [512, 512], P(None, 'tp'), may hold values from -0.25 to 0.25
- out_broad: bfloat16 [1024, 2048], replicated, may hold values from -0.15625 to 0.15625
- out_narrow: bfloat16 [512, 2048], replicated, may hold values from -0.15625 to 0.15625
- post_gain: float32 [2048], replicated, may hold values from 0.1 to 1.9
- ffn_gain: float32 [2048], replicated, may hold values from 0.1 to 1.9
- up_weight: bfloat16 [2048, 8192], P('sp', 'tp'), may hold values from -0.125 to 0.125
- down_weight: bfloat16 [2048, 8192], P('sp', 'tp'), may hold values from -0.0625 to 0.0625
- ffn_out_gain: float32 [2048], replicated, may hold values from 0.1 to 1.9
Outputs:
- layer_out: bfloat16 [1536, 2048], P(('sp', 'tp'))
The draws below stay inside these ranges and needn't reach their ends.
All inputs are finite; a program needn't handle non-finite values.
Results may differ from the reference program's by a relative error of at most 0.013.
Values may be sent and summed in bfloat16 or wider, within the bound.
A program may use at most 128 MiB of HBM per device.

```python
import math
import jax
import jax.numpy as jnp
from jax import lax

D = 2048
FF = 8192
R = 512
ROPE = 64
DB = 128
DN = 64
HB = 8
HN = 8
SEQ = 1536


def drawn_queries(key, salt, head_count, head_size):
    drawn = jax.random.normal(jax.random.fold_in(key, salt), (SEQ, head_count, head_size + ROPE), jnp.float32)
    return jnp.clip(drawn, -6.0, 6.0)


def draw_query_broad(key, part):
    entries = drawn_queries(key, 21, HB, DB)
    return entries.reshape(SEQ, HB * (DB + ROPE)).astype(jnp.bfloat16)


def draw_query_narrow(key, part):
    entries = drawn_queries(key, 31, HN, DN)
    return entries.reshape(SEQ, HN * (DN + ROPE)).astype(jnp.bfloat16)


def draw_key_rope(key, part):
    entries = jnp.clip(jax.random.normal(jax.random.fold_in(key, 11), (SEQ, ROPE), jnp.float32), -6.0, 6.0)
    return entries.astype(jnp.bfloat16)


def block_scale(rng, dims, cuts, least, top_value):
    def one(dim, shards_of):
        heights = jax.random.uniform(jax.random.fold_in(jax.random.fold_in(rng, 6), dim), (shards_of,), jnp.float32, least / len(cuts), top_value / len(cuts))
        return jnp.repeat(jnp.exp(heights), dims[dim] // shards_of).reshape((-1,) + (1,) * (len(dims) - dim - 1))

    factor_of = one(*cuts[0])
    for cut in cuts[1:]:
        factor_of = factor_of * one(*cut)
    return factor_of


def bell_draw(rng, extent, width, reach, cuts=(), held_as=jnp.bfloat16):
    factor_of = block_scale(rng, extent, cuts, -0.22, 0.18) if cuts else 1.0
    result = jax.random.normal(rng, extent, jnp.float32) * width * factor_of
    return jnp.minimum(jnp.maximum(result, -reach), reach).astype(held_as)


def setup_inputs(seed: int = 0) -> dict:
    streams_of = jax.random.split(jax.random.key(seed), 18)
    return {
        "resid": bell_draw(streams_of[0], (SEQ, D), 1.0, 6.0, ((0, 8),)),
        "query_broad": draw_query_broad(jax.random.fold_in(streams_of[17], 71), 0),
        "query_narrow": draw_query_narrow(jax.random.fold_in(streams_of[17], 71), 0),
        "latent": bell_draw(streams_of[3], (SEQ, R), 1.0, 6.0, ((0, 8),)),
        "key_rope": draw_key_rope(jax.random.fold_in(streams_of[17], 71), 0),
        "latent_gain": jnp.clip(1.0 + 0.18 * jax.random.normal(streams_of[5], (R,), jnp.float32), 0.1, 1.9),
        "key_up_broad": bell_draw(streams_of[6], (R, HB * DB), R ** -0.5, 0.25, ((1, 4),)),
        "value_up_broad": bell_draw(streams_of[7], (R, HB * DB), R ** -0.5, 0.25, ((1, 4),)),
        "key_up_narrow": bell_draw(streams_of[8], (R, HN * DN), R ** -0.5, 0.25, ((1, 4),)),
        "value_up_narrow": bell_draw(streams_of[9], (R, HN * DN), R ** -0.5, 0.25, ((1, 4),)),
        "out_broad": bell_draw(streams_of[10], (HB * DB, D), (HB * DB + HN * DN) ** -0.5, 0.15625),
        "out_narrow": bell_draw(streams_of[11], (HN * DN, D), (HB * DB + HN * DN) ** -0.5, 0.15625),
        "post_gain": jnp.clip(1.0 + 0.18 * jax.random.normal(streams_of[12], (D,), jnp.float32), 0.1, 1.9),
        "ffn_gain": jnp.clip(1.0 + 0.18 * jax.random.normal(streams_of[13], (D,), jnp.float32), 0.1, 1.9),
        "up_weight": bell_draw(streams_of[14], (D, FF), D ** -0.5, 0.125, ((0, 8), (1, 4))),
        "down_weight": bell_draw(streams_of[15], (D, FF), FF ** -0.5, 0.0625, ((0, 8), (1, 4))),
        "ffn_out_gain": jnp.clip(1.0 + 0.18 * jax.random.normal(streams_of[16], (D,), jnp.float32), 0.1, 1.9),
    }


norm_eps = 1e-06
rope_base = 500000.0
masked_score = -1e+30

def rotate(values, positions):
    full_width = values.shape[-1]
    half_width = full_width // 2
    frequency = rope_base ** (-2.0 * jnp.arange(half_width, dtype=jnp.float32) / full_width)
    angles = positions.astype(jnp.float32)[:, None] * frequency[None, :]
    angle_shape = (angles.shape[0],) + (1,) * (values.ndim - 2) + (half_width,)
    cosine = jnp.cos(angles).reshape(angle_shape)
    sine_part = jnp.sin(angles).reshape(angle_shape)
    leading = values[..., :half_width]
    trailing = values[..., half_width:]
    return jnp.concatenate([leading * cosine - trailing * sine_part, trailing * cosine + leading * sine_part], axis=-1)

def rms_scale(values, norm_gain):
    return values * lax.rsqrt(lax.optimization_barrier(jnp.mean(values * values, axis=-1, keepdims=True)) + norm_eps) * norm_gain

def attend_all(query_nope, query_rope, key_rows, key_rot, value_rows, score_scale):
    block_rows = math.gcd(SEQ, 512)
    positions = jnp.arange(SEQ, dtype=jnp.int32)
    keys_wide = key_rows.astype(jnp.float32)
    rot_wide = key_rot.astype(jnp.float32)
    values_wide = value_rows.astype(jnp.float32)

    def one_block(block_index):
        begin = block_index * block_rows
        nope_part = lax.dynamic_slice_in_dim(query_nope, begin, block_rows, 0).astype(jnp.float32)
        rope_part = lax.dynamic_slice_in_dim(query_rope, begin, block_rows, 0).astype(jnp.float32)
        query_pos = begin + jnp.arange(block_rows, dtype=jnp.int32)
        scores = jnp.einsum('qhd,khd->hqk', nope_part, keys_wide) + jnp.einsum('qhd,kd->hqk', rope_part, rot_wide)
        scores = scores * score_scale
        allowed = (positions[None, :] <= query_pos[:, None])[None]
        scores = jnp.where(allowed, scores, masked_score)
        highest = lax.optimization_barrier(jnp.max(scores, axis=-1, keepdims=True))
        exponent = jnp.where(allowed, jnp.exp(scores - highest), 0.0)
        denominator = lax.optimization_barrier(jnp.sum(exponent, axis=-1))
        rounded = lax.optimization_barrier(exponent.astype(jnp.bfloat16)).astype(jnp.float32)
        summed = jnp.einsum('hqk,khd->qhd', rounded, values_wide)
        return (summed / jnp.transpose(denominator)[:, :, None]).astype(jnp.bfloat16)
    heads_out = lax.map(one_block, jnp.arange(SEQ // block_rows, dtype=jnp.int32))
    return heads_out.reshape(SEQ, value_rows.shape[1] * value_rows.shape[2])

def reference(resid, query_broad, query_narrow, latent, key_rope, latent_gain, key_up_broad, value_up_broad, key_up_narrow, value_up_narrow, out_broad, out_narrow, post_gain, ffn_gain, up_weight, down_weight, ffn_out_gain):
    positions = jnp.arange(SEQ, dtype=jnp.int32)
    latent_normed = rms_scale(latent.astype(jnp.float32), latent_gain).astype(jnp.bfloat16)

    def expand(weight, head_size):
        product = jnp.dot(latent_normed, weight, preferred_element_type=jnp.float32)
        return product.astype(jnp.bfloat16).reshape(SEQ, -1, head_size)
    key_broad = expand(key_up_broad, DB)
    value_broad = expand(value_up_broad, DB)
    key_narrow = expand(key_up_narrow, DN)
    value_narrow = expand(value_up_narrow, DN)
    key_rot = rotate(key_rope.astype(jnp.float32), positions).astype(jnp.bfloat16)
    broad_heads = query_broad.reshape(SEQ, HB, DB + ROPE)
    broad_rope = rotate(broad_heads[:, :, DB:].astype(jnp.float32), positions).astype(jnp.bfloat16)
    narrow_heads = query_narrow.reshape(SEQ, HN, DN + ROPE)
    narrow_rope = rotate(narrow_heads[:, :, DN:].astype(jnp.float32), positions).astype(jnp.bfloat16)
    attn_broad = attend_all(broad_heads[:, :, :DB], broad_rope, key_broad, key_rot, value_broad, (DB + ROPE) ** (-0.5))
    attn_narrow = attend_all(narrow_heads[:, :, :DN], narrow_rope, key_narrow, key_rot, value_narrow, (DN + ROPE) ** (-0.5))
    projected = jnp.dot(attn_broad, out_broad, preferred_element_type=jnp.float32) + jnp.dot(attn_narrow, out_narrow, preferred_element_type=jnp.float32)
    mixed = (resid.astype(jnp.float32) + rms_scale(projected, post_gain)).astype(jnp.bfloat16)
    normed = rms_scale(mixed.astype(jnp.float32), ffn_gain).astype(jnp.bfloat16)
    hidden = jnp.square(jax.nn.relu(jnp.dot(normed, up_weight, preferred_element_type=jnp.float32))).astype(jnp.bfloat16)
    ffn = lax.dot_general(hidden, down_weight, (((1,), (1,)), ((), ())), preferred_element_type=jnp.float32)
    return (mixed.astype(jnp.float32) + rms_scale(ffn, ffn_out_gain)).astype(jnp.bfloat16)
```

```python
import math

import jax
import jax.numpy as jnp
from jax import lax
from jax.experimental import pallas as pl
from jax.experimental.pallas import tpu as pltpu
from jax.sharding import PartitionSpec as P

DB = 128
DN = 64


norm_eps = 1e-06
rope_base = 500000.0
masked_score = -1e30


def rotate(values, positions):
    full_width = values.shape[-1]
    half_width = full_width // 2
    frequency = rope_base ** (-2.0 * jnp.arange(half_width, dtype=jnp.float32) / full_width)
    angles = positions.astype(jnp.float32)[:, None] * frequency[None, :]
    angle_shape = (angles.shape[0],) + (1,) * (values.ndim - 2) + (half_width,)
    cosine = jnp.cos(angles).reshape(angle_shape)
    sine_part = jnp.sin(angles).reshape(angle_shape)
    leading = values[..., :half_width]
    trailing = values[..., half_width:]
    return jnp.concatenate(
        [leading * cosine - trailing * sine_part, trailing * cosine + leading * sine_part], axis=-1
    )


def rms_scale(values, norm_gain):
    return (
        values * lax.rsqrt(jnp.mean(values * values, axis=-1, keepdims=True) + norm_eps) * norm_gain
    )


def group_update(
    running, nope_query, rope_query, key_rows, key_rot, value_rows, score_scale, allowed
):
    old_max, old_sum, old_acc = running
    scores = jnp.einsum("qhd,khd->hqk", nope_query, key_rows, preferred_element_type=jnp.float32)
    scores = scores + jnp.einsum(
        "qhd,kd->hqk", rope_query, key_rot, preferred_element_type=jnp.float32
    )
    scores = jnp.where(allowed, scores * score_scale, masked_score)
    new_max = jnp.maximum(old_max, jnp.max(scores, axis=-1))
    exponent = jnp.where(allowed, jnp.exp(scores - new_max[:, :, None]), 0.0)
    factor = jnp.exp(old_max - new_max)
    new_sum = old_sum * factor + jnp.sum(exponent, axis=-1)
    weighted = jnp.einsum(
        "hqk,khd->qhd",
        exponent.astype(jnp.bfloat16),
        value_rows,
        preferred_element_type=jnp.float32,
    )
    new_acc = old_acc * jnp.transpose(factor)[:, :, None] + weighted
    return (new_max, new_sum, new_acc)


def local(
    resid,
    query_broad,
    query_narrow,
    latent,
    key_rope,
    latent_gain,
    key_up_broad,
    value_up_broad,
    key_up_narrow,
    value_up_narrow,
    out_broad,
    out_narrow,
    post_gain,
    ffn_gain,
    up_weight,
    down_weight,
    ffn_out_gain,
):
    local_rows = resid.shape[0]
    head_parts = lax.axis_size("tp")
    share_rows = local_rows // head_parts
    row_offset = lax.axis_index("sp") * local_rows
    last_query = row_offset + local_rows - 1
    query_pos = row_offset + jnp.arange(local_rows, dtype=jnp.int32)
    rope_width = key_rope.shape[1]
    broad_count = key_up_broad.shape[1] // DB
    narrow_count = key_up_narrow.shape[1] // DN
    broad_heads = query_broad.reshape(local_rows, broad_count, DB + rope_width)
    broad_nope = broad_heads[:, :, :DB]
    broad_rope = rotate(broad_heads[:, :, DB:].astype(jnp.float32), query_pos).astype(jnp.bfloat16)
    narrow_heads = query_narrow.reshape(local_rows, narrow_count, DN + rope_width)
    narrow_nope = narrow_heads[:, :, :DN]
    narrow_rope = rotate(narrow_heads[:, :, DN:].astype(jnp.float32), query_pos).astype(
        jnp.bfloat16
    )
    broad_scale = (DB + rope_width) ** (-0.5)
    narrow_scale = (DN + rope_width) ** (-0.5)

    def attend(running, latent_rows, rope_rows, first_row):
        key_count = latent_rows.shape[0]
        key_pos = first_row + jnp.arange(key_count, dtype=jnp.int32)
        latent_normed = rms_scale(latent_rows.astype(jnp.float32), latent_gain).astype(jnp.bfloat16)

        def expand(weight, head_size):
            product = jnp.dot(latent_normed, weight, preferred_element_type=jnp.float32)
            return product.astype(jnp.bfloat16).reshape(key_count, -1, head_size)

        key_rot = rotate(rope_rows.astype(jnp.float32), key_pos).astype(jnp.bfloat16)
        allowed = (key_pos[None, :] <= query_pos[:, None])[None]
        broad_state = group_update(
            running[0],
            broad_nope,
            broad_rope,
            expand(key_up_broad, DB),
            key_rot,
            expand(value_up_broad, DB),
            broad_scale,
            allowed,
        )
        narrow_state = group_update(
            running[1],
            narrow_nope,
            narrow_rope,
            expand(key_up_narrow, DN),
            key_rot,
            expand(value_up_narrow, DN),
            narrow_scale,
            allowed,
        )
        return (broad_state, narrow_state)

    def fresh(head_count, head_size):
        return (
            jnp.full((head_count, local_rows), masked_score, jnp.float32),
            jnp.zeros((head_count, local_rows), jnp.float32),
            jnp.zeros((local_rows, head_count, head_size), jnp.float32),
        )

    initial = (fresh(broad_count, DB), fresh(narrow_count, DN))
    latent_piece = lax.all_gather(latent, "sp", axis=0, tiled=True)
    rope_piece = lax.all_gather(key_rope, "sp", axis=0, tiled=True)
    piece_rows = latent_piece.shape[0]
    block_rows = math.gcd(piece_rows, 1024)

    def one_block(block_index, carried):
        begin = block_index * block_rows
        latent_block = lax.dynamic_slice_in_dim(latent_piece, begin, block_rows, 0)
        rope_block = lax.dynamic_slice_in_dim(rope_piece, begin, block_rows, 0)

        def unchanged(kept_state):
            return kept_state

        def updated(kept_state):
            return attend(kept_state, latent_block, rope_block, begin)

        return lax.cond(begin > last_query, unchanged, updated, carried)

    final_state = lax.fori_loop(0, piece_rows // block_rows, one_block, initial)

    def finish(running):
        run_max, run_sum, run_acc = running
        return (
            (run_acc / jnp.transpose(run_sum)[:, :, None])
            .astype(jnp.bfloat16)
            .reshape(local_rows, -1)
        )

    attn_broad = finish(final_state[0])
    attn_narrow = finish(final_state[1])
    rows_broad, rows_narrow = (
        lax.all_to_all(attn_broad, "tp", split_axis=0, concat_axis=1, tiled=True),
        lax.all_to_all(attn_narrow, "tp", split_axis=0, concat_axis=1, tiled=True),
    )
    projected = jnp.dot(rows_broad, out_broad, preferred_element_type=jnp.float32) + jnp.dot(
        rows_narrow, out_narrow, preferred_element_type=jnp.float32
    )
    own_resid = lax.dynamic_slice_in_dim(resid, lax.axis_index("tp") * share_rows, share_rows, 0)
    mixed = (own_resid.astype(jnp.float32) + rms_scale(projected, post_gain)).astype(jnp.bfloat16)
    normed = rms_scale(mixed.astype(jnp.float32), ffn_gain).astype(jnp.bfloat16)
    up_full, down_full = (
        lax.all_gather(up_weight, "sp", axis=0, tiled=True),
        lax.all_gather(down_weight, "sp", axis=0, tiled=True),
    )
    hidden = jnp.square(
        jax.nn.relu(
            jnp.dot(
                lax.all_gather(normed, "tp", axis=0, tiled=True),
                up_full,
                preferred_element_type=jnp.float32,
            )
        )
    ).astype(jnp.bfloat16)
    ffn = lax.psum_scatter(
        lax.dot_general(
            hidden, down_full, (((1,), (1,)), ((), ())), preferred_element_type=jnp.float32
        ).astype(jnp.bfloat16),
        "tp",
        scatter_dimension=0,
        tiled=True,
    ).astype(jnp.float32)
    return (mixed.astype(jnp.float32) + rms_scale(ffn, ffn_out_gain)).astype(jnp.bfloat16)


lane_tile = 128
row_parts = 2


def attend_kernel(qb_ref, qn_ref, lat_ref, rot_ref, kb_ref, vb_ref, kn_ref, vn_ref, o_ref):
    rows = qb_ref.shape[0]
    total = lat_ref.shape[0]
    rope = rot_ref.shape[1]
    block = 2 * rows
    broad = kb_ref.shape[1] // DB
    narrow = kn_ref.shape[1] // DN
    first = lax.axis_index("sp") * rows
    blocks = lax.div(first + rows + block - 1, block)
    query_pos = first + lax.broadcasted_iota(jnp.int32, (rows, block), 0)
    key_iota = lax.broadcasted_iota(jnp.int32, (rows, block), 1)
    wb = DB + rope
    wn = DN + rope
    heads = broad + narrow
    widths = [DB] * broad + [narrow * DN] * narrow

    def step(index, carried):
        start = pl.multiple_of(index * block, block)
        lat = lat_ref[pl.ds(start, block), :]
        rot = rot_ref[pl.ds(start, block), :]

        def expand(ref):
            return jnp.dot(lat, ref[...], preferred_element_type=jnp.float32).astype(jnp.bfloat16)

        kb, vb, kn, vn = expand(kb_ref), expand(vb_ref), expand(kn_ref), expand(vn_ref)
        allowed = key_iota + start <= query_pos
        out = []
        for h in range(heads):
            old_max, old_sum, old_acc = carried[h]
            if h < broad:
                q = qb_ref[:, h * wb : (h + 1) * wb]
                k = jnp.concatenate([kb[:, h * DB : (h + 1) * DB], rot], axis=1)
                v = vb[:, h * DB : (h + 1) * DB]
                scale = wb ** (-0.5)
            else:
                n = h - broad
                q = qn_ref[:, n * wn : (n + 1) * wn]
                k = jnp.concatenate([kn[:, n * DN : (n + 1) * DN], rot], axis=1)
                v = vn
                scale = wn ** (-0.5)
            s = lax.dot_general(
                q, k, (((1,), (1,)), ((), ())), preferred_element_type=jnp.float32
            )
            s = jnp.where(allowed, s * scale, masked_score)
            new_max = jnp.maximum(old_max, jnp.max(s, axis=-1, keepdims=True))
            e = jnp.where(allowed, jnp.exp(s - new_max), 0.0)
            factor = jnp.exp(old_max - new_max)
            new_sum = old_sum * factor + jnp.sum(e, axis=-1, keepdims=True)
            pv = jnp.dot(e.astype(jnp.bfloat16), v, preferred_element_type=jnp.float32)
            out.append((new_max, new_sum, old_acc * factor + pv))
        return tuple(out)

    init = tuple(
        (
            jnp.full((rows, 1), masked_score, jnp.float32),
            jnp.zeros((rows, 1), jnp.float32),
            jnp.zeros((rows, w), jnp.float32),
        )
        for w in widths
    )
    final = lax.fori_loop(0, blocks, step, init)
    parts = [final[h][2] / final[h][1] for h in range(heads)]
    for h in range(broad):
        o_ref[:, h * DB : (h + 1) * DB] = parts[h].astype(o_ref.dtype)
    if narrow:
        column = lax.broadcasted_iota(jnp.int32, parts[broad].shape, 1)
        mixed = parts[broad]
        for n in range(1, narrow):
            mixed = jnp.where(column >= n * DN, parts[broad + n], mixed)
        o_ref[:, broad * DB :] = mixed.astype(o_ref.dtype)


def fast_local(
    resid,
    query_broad,
    query_narrow,
    latent,
    key_rope,
    latent_gain,
    key_up_broad,
    value_up_broad,
    key_up_narrow,
    value_up_narrow,
    out_broad,
    out_narrow,
    post_gain,
    ffn_gain,
    up_weight,
    down_weight,
    ffn_out_gain,
):
    sp = lax.axis_size("sp")
    tp = lax.axis_size("tp")
    cols = row_parts
    lines = sp // cols
    s = lax.axis_index("sp")
    z = s // cols
    y = s % cols
    local_rows = resid.shape[0]
    share_rows = local_rows // tp
    query_pos = s * local_rows + jnp.arange(local_rows, dtype=jnp.int32)
    rope_width = key_rope.shape[1]
    bf16 = jnp.bfloat16

    def shift_line(values, k):
        pairs = [
            (a * cols + b, ((a + k) % lines) * cols + b)
            for a in range(lines)
            for b in range(cols)
        ]
        return lax.ppermute(values, "sp", pairs)

    def swap_col(values):
        return lax.ppermute(values, "sp", [(i, i ^ 1) for i in range(sp)])

    def flip(values, bit):
        return lax.ppermute(values, "tp", [(i, i ^ bit) for i in range(tp)])

    normed_latent = rms_scale(latent.astype(jnp.float32), latent_gain).astype(bf16)
    key_rot = rotate(key_rope.astype(jnp.float32), query_pos).astype(bf16)
    both = jnp.concatenate([normed_latent, key_rot], axis=1)
    core = lax.axis_index("tp") % 2
    half_rows = local_rows // 2
    mine = lax.dynamic_slice_in_dim(both, core * half_rows, half_rows, 0)
    gathered = jnp.zeros((sp, half_rows, both.shape[1]), bf16)
    for k in range(lines):
        piece = mine if k == 0 else shift_line(mine, k)
        source = ((z - k) % lines) * cols
        gathered = lax.dynamic_update_slice(gathered, piece[None], (source + y, 0, 0))
        gathered = lax.dynamic_update_slice(
            gathered, swap_col(piece)[None], (source + (1 - y), 0, 0)
        )
    other = flip(gathered, 1)
    first_half = jnp.where(core == 0, gathered, other)
    second_half = jnp.where(core == 0, other, gathered)
    everything = jnp.concatenate([first_half, second_half], axis=1).reshape(
        sp * local_rows, both.shape[1]
    )
    latents = everything[:, : latent.shape[1]]
    rots = everything[:, latent.shape[1] :]

    def rotate_queries(queries, head_size):
        parts = queries.reshape(local_rows, -1, head_size + rope_width)
        rotated = rotate(parts[:, :, head_size:].astype(jnp.float32), query_pos).astype(bf16)
        return jnp.concatenate([parts[:, :, :head_size], rotated], axis=-1).reshape(queries.shape)

    broad_width = key_up_broad.shape[1]
    narrow_width = key_up_narrow.shape[1]
    width = broad_width + narrow_width
    attn = pl.pallas_call(
        attend_kernel,
        out_shape=jax.ShapeDtypeStruct((local_rows, width), bf16),
        in_specs=[pl.BlockSpec(memory_space=pltpu.VMEM)] * 8,
        out_specs=pl.BlockSpec(memory_space=pltpu.VMEM),
        cost_estimate=pl.CostEstimate(
            flops=8 * local_rows * sp * local_rows * width, bytes_accessed=0, transcendentals=0
        ),
    )(
        rotate_queries(query_broad, DB),
        rotate_queries(query_narrow, DN),
        latents,
        rots,
        key_up_broad,
        value_up_broad,
        key_up_narrow,
        value_up_narrow,
    )
    rows = lax.all_to_all(attn, "tp", split_axis=0, concat_axis=1, tiled=True)
    rows = rows.reshape(share_rows, tp, width)
    rows_broad = rows[:, :, :broad_width].reshape(share_rows, -1)
    rows_narrow = rows[:, :, broad_width:].reshape(share_rows, -1)
    projected = jnp.dot(rows_broad, out_broad, preferred_element_type=jnp.float32) + jnp.dot(
        rows_narrow, out_narrow, preferred_element_type=jnp.float32
    )
    own_resid = lax.dynamic_slice_in_dim(resid, lax.axis_index("tp") * share_rows, share_rows, 0)
    mixed = (own_resid.astype(jnp.float32) + rms_scale(projected, post_gain)).astype(bf16)
    normed = rms_scale(mixed.astype(jnp.float32), ffn_gain).astype(bf16)

    slice_width = up_weight.shape[1] // lines

    def spread(weight):
        held = jnp.zeros((sp, weight.shape[0], slice_width), bf16)
        for k in range(lines):
            target = ((z + k) % lines) * slice_width
            piece = lax.dynamic_slice_in_dim(weight, target, slice_width, 1)
            if k:
                piece = shift_line(piece, k)
            source = ((z - k) % lines) * cols
            held = lax.dynamic_update_slice(held, piece[None], (source + y, 0, 0))
            held = lax.dynamic_update_slice(
                held, swap_col(piece)[None], (source + (1 - y), 0, 0)
            )
        return held.reshape(-1, slice_width)

    up_part = spread(up_weight)
    down_part = spread(down_weight)
    pieces = [normed] + [shift_line(normed, k) for k in range(1, lines)]
    bit = tp // 2
    while bit > 1:
        pieces = pieces + [flip(piece, bit) for piece in pieces]
        bit //= 2
    near = jnp.concatenate(pieces, axis=0)
    far = flip(near, 1)

    def feed(block):
        product = jnp.dot(block, up_part, preferred_element_type=jnp.float32)
        hidden = jnp.square(jax.nn.relu(product)).astype(bf16)
        return lax.dot_general(
            hidden, down_part, (((1,), (1,)), ((), ())), preferred_element_type=jnp.float32
        )

    far_sum = flip(feed(far).astype(bf16), 1)
    total = feed(near) + far_sum.astype(jnp.float32)
    bit = 2
    while bit < tp:
        half = total.shape[0] // 2
        sent = total[half:].astype(bf16)
        got = jnp.concatenate(
            [
                flip(sent[i : i + share_rows], bit)
                for i in range(0, half, share_rows)
            ],
            axis=0,
        )
        total = total[:half] + got.astype(jnp.float32)
        bit *= 2
    ffn = total[:share_rows]
    for k in range(1, lines):
        sent = total[k * share_rows : (k + 1) * share_rows].astype(bf16)
        ffn = ffn + shift_line(sent, -k).astype(jnp.float32)
    return (mixed.astype(jnp.float32) + rms_scale(ffn, ffn_out_gain)).astype(bf16)


def solution(mesh):
    in_specs = (
        P("sp", None),
        P("sp", "tp"),
        P("sp", "tp"),
        P("sp", None),
        P("sp", None),
        P(),
        P(None, "tp"),
        P(None, "tp"),
        P(None, "tp"),
        P(None, "tp"),
        P(),
        P(),
        P(),
        P(),
        P("sp", "tp"),
        P("sp", "tp"),
        P(),
    )
    out_specs = P(("sp", "tp"), None)
    sp = mesh.shape["sp"]
    tp = mesh.shape["tp"]

    def whole(*args):
        hidden = args[14].shape[1] // tp
        rows = args[0].shape[0] // sp
        lines = sp // row_parts
        fits = (
            sp % row_parts == 0
            and tp & (tp - 1) == 0
            and tp > 1
            and lines > 1
            and hidden % (lines * lane_tile) == 0
            and rows % (16 * tp) == 0
        )
        body = fast_local if fits else local
        return jax.shard_map(
            body, mesh=mesh, in_specs=in_specs, out_specs=out_specs, check_vma=False
        )(*args)

    return whole
```

```python
import functools
import math

import jax
import jax.numpy as jnp
from jax import lax
from jax.experimental import pallas as pl
from jax.experimental.pallas import tpu as pltpu
from jax.sharding import PartitionSpec as P

DB = 128
DN = 64


norm_eps = 1e-06
rope_base = 500000.0
masked_score = -1e30


def rotate(values, positions):
    full_width = values.shape[-1]
    half_width = full_width // 2
    frequency = rope_base ** (-2.0 * jnp.arange(half_width, dtype=jnp.float32) / full_width)
    angles = positions.astype(jnp.float32)[:, None] * frequency[None, :]
    angle_shape = (angles.shape[0],) + (1,) * (values.ndim - 2) + (half_width,)
    cosine = jnp.cos(angles).reshape(angle_shape)
    sine_part = jnp.sin(angles).reshape(angle_shape)
    leading = values[..., :half_width]
    trailing = values[..., half_width:]
    return jnp.concatenate(
        [leading * cosine - trailing * sine_part, trailing * cosine + leading * sine_part], axis=-1
    )


def rms_scale(values, norm_gain):
    return (
        values * lax.rsqrt(jnp.mean(values * values, axis=-1, keepdims=True) + norm_eps) * norm_gain
    )


def group_update(
    running, nope_query, rope_query, key_rows, key_rot, value_rows, score_scale, allowed
):
    old_max, old_sum, old_acc = running
    scores = jnp.einsum("qhd,khd->hqk", nope_query, key_rows, preferred_element_type=jnp.float32)
    scores = scores + jnp.einsum(
        "qhd,kd->hqk", rope_query, key_rot, preferred_element_type=jnp.float32
    )
    scores = jnp.where(allowed, scores * score_scale, masked_score)
    new_max = jnp.maximum(old_max, jnp.max(scores, axis=-1))
    exponent = jnp.where(allowed, jnp.exp(scores - new_max[:, :, None]), 0.0)
    factor = jnp.exp(old_max - new_max)
    new_sum = old_sum * factor + jnp.sum(exponent, axis=-1)
    weighted = jnp.einsum(
        "hqk,khd->qhd",
        exponent.astype(jnp.bfloat16),
        value_rows,
        preferred_element_type=jnp.float32,
    )
    new_acc = old_acc * jnp.transpose(factor)[:, :, None] + weighted
    return (new_max, new_sum, new_acc)


def local(
    resid,
    query_broad,
    query_narrow,
    latent,
    key_rope,
    latent_gain,
    key_up_broad,
    value_up_broad,
    key_up_narrow,
    value_up_narrow,
    out_broad,
    out_narrow,
    post_gain,
    ffn_gain,
    up_weight,
    down_weight,
    ffn_out_gain,
):
    local_rows = resid.shape[0]
    head_parts = lax.axis_size("tp")
    share_rows = local_rows // head_parts
    row_offset = lax.axis_index("sp") * local_rows
    last_query = row_offset + local_rows - 1
    query_pos = row_offset + jnp.arange(local_rows, dtype=jnp.int32)
    rope_width = key_rope.shape[1]
    broad_count = key_up_broad.shape[1] // DB
    narrow_count = key_up_narrow.shape[1] // DN
    broad_heads = query_broad.reshape(local_rows, broad_count, DB + rope_width)
    broad_nope = broad_heads[:, :, :DB]
    broad_rope = rotate(broad_heads[:, :, DB:].astype(jnp.float32), query_pos).astype(jnp.bfloat16)
    narrow_heads = query_narrow.reshape(local_rows, narrow_count, DN + rope_width)
    narrow_nope = narrow_heads[:, :, :DN]
    narrow_rope = rotate(narrow_heads[:, :, DN:].astype(jnp.float32), query_pos).astype(
        jnp.bfloat16
    )
    broad_scale = (DB + rope_width) ** (-0.5)
    narrow_scale = (DN + rope_width) ** (-0.5)

    def attend(running, latent_rows, rope_rows, first_row):
        key_count = latent_rows.shape[0]
        key_pos = first_row + jnp.arange(key_count, dtype=jnp.int32)
        latent_normed = rms_scale(latent_rows.astype(jnp.float32), latent_gain).astype(jnp.bfloat16)

        def expand(weight, head_size):
            product = jnp.dot(latent_normed, weight, preferred_element_type=jnp.float32)
            return product.astype(jnp.bfloat16).reshape(key_count, -1, head_size)

        key_rot = rotate(rope_rows.astype(jnp.float32), key_pos).astype(jnp.bfloat16)
        allowed = (key_pos[None, :] <= query_pos[:, None])[None]
        broad_state = group_update(
            running[0],
            broad_nope,
            broad_rope,
            expand(key_up_broad, DB),
            key_rot,
            expand(value_up_broad, DB),
            broad_scale,
            allowed,
        )
        narrow_state = group_update(
            running[1],
            narrow_nope,
            narrow_rope,
            expand(key_up_narrow, DN),
            key_rot,
            expand(value_up_narrow, DN),
            narrow_scale,
            allowed,
        )
        return (broad_state, narrow_state)

    def fresh(head_count, head_size):
        return (
            jnp.full((head_count, local_rows), masked_score, jnp.float32),
            jnp.zeros((head_count, local_rows), jnp.float32),
            jnp.zeros((local_rows, head_count, head_size), jnp.float32),
        )

    initial = (fresh(broad_count, DB), fresh(narrow_count, DN))
    latent_piece = lax.all_gather(latent, "sp", axis=0, tiled=True)
    rope_piece = lax.all_gather(key_rope, "sp", axis=0, tiled=True)
    piece_rows = latent_piece.shape[0]
    block_rows = math.gcd(piece_rows, 1024)

    def one_block(block_index, carried):
        begin = block_index * block_rows
        latent_block = lax.dynamic_slice_in_dim(latent_piece, begin, block_rows, 0)
        rope_block = lax.dynamic_slice_in_dim(rope_piece, begin, block_rows, 0)

        def unchanged(kept_state):
            return kept_state

        def updated(kept_state):
            return attend(kept_state, latent_block, rope_block, begin)

        return lax.cond(begin > last_query, unchanged, updated, carried)

    final_state = lax.fori_loop(0, piece_rows // block_rows, one_block, initial)

    def finish(running):
        run_max, run_sum, run_acc = running
        return (
            (run_acc / jnp.transpose(run_sum)[:, :, None])
            .astype(jnp.bfloat16)
            .reshape(local_rows, -1)
        )

    attn_broad = finish(final_state[0])
    attn_narrow = finish(final_state[1])
    rows_broad, rows_narrow = (
        lax.all_to_all(attn_broad, "tp", split_axis=0, concat_axis=1, tiled=True),
        lax.all_to_all(attn_narrow, "tp", split_axis=0, concat_axis=1, tiled=True),
    )
    projected = jnp.dot(rows_broad, out_broad, preferred_element_type=jnp.float32) + jnp.dot(
        rows_narrow, out_narrow, preferred_element_type=jnp.float32
    )
    own_resid = lax.dynamic_slice_in_dim(resid, lax.axis_index("tp") * share_rows, share_rows, 0)
    mixed = (own_resid.astype(jnp.float32) + rms_scale(projected, post_gain)).astype(jnp.bfloat16)
    normed = rms_scale(mixed.astype(jnp.float32), ffn_gain).astype(jnp.bfloat16)
    up_full, down_full = (
        lax.all_gather(up_weight, "sp", axis=0, tiled=True),
        lax.all_gather(down_weight, "sp", axis=0, tiled=True),
    )
    hidden = jnp.square(
        jax.nn.relu(
            jnp.dot(
                lax.all_gather(normed, "tp", axis=0, tiled=True),
                up_full,
                preferred_element_type=jnp.float32,
            )
        )
    ).astype(jnp.bfloat16)
    ffn = lax.psum_scatter(
        lax.dot_general(
            hidden, down_full, (((1,), (1,)), ((), ())), preferred_element_type=jnp.float32
        ).astype(jnp.bfloat16),
        "tp",
        scatter_dimension=0,
        tiled=True,
    ).astype(jnp.float32)
    return (mixed.astype(jnp.float32) + rms_scale(ffn, ffn_out_gain)).astype(jnp.bfloat16)

lane_tile = 128
row_parts = 2


def attend_rows(qb_ref, qn_ref, lat_ref, kb_ref, vb_ref, kn_ref, vn_ref, o_ref):
    rows = qb_ref.shape[0]
    latent_width = kb_ref.shape[0]
    rope = lat_ref.shape[3] - latent_width
    share = o_ref.shape[1]
    block = 2 * rows
    broad = kb_ref.shape[1] // DB
    narrow = kn_ref.shape[1] // DN
    first = lax.axis_index("sp") * rows
    blocks = lax.div(first + rows + block - 1, block)
    query_pos = first + lax.broadcasted_iota(jnp.int32, (rows, block), 0)
    key_iota = lax.broadcasted_iota(jnp.int32, (rows, block), 1)
    wb = DB + rope
    wn = DN + rope
    heads = broad + narrow
    widths = [DB] * broad + [narrow * DN] * narrow

    def step(index, carried):
        start = pl.multiple_of(index * block, block)
        both = lat_ref[pl.ds(2 * index, 2)].reshape(block, latent_width + rope)
        lat = both[:, :latent_width]
        rot = both[:, latent_width:]

        def expand(ref):
            return jnp.dot(lat, ref[...], preferred_element_type=jnp.float32).astype(jnp.bfloat16)

        kb, vb, kn, vn = expand(kb_ref), expand(vb_ref), expand(kn_ref), expand(vn_ref)
        allowed = key_iota + start <= query_pos
        out = []
        for h in range(heads):
            old_max, old_sum, old_acc = carried[h]
            if h < broad:
                q = qb_ref[:, h * wb : (h + 1) * wb]
                k = jnp.concatenate([kb[:, h * DB : (h + 1) * DB], rot], axis=1)
                v = vb[:, h * DB : (h + 1) * DB]
                scale = wb ** (-0.5)
            else:
                n = h - broad
                q = qn_ref[:, n * wn : (n + 1) * wn]
                k = jnp.concatenate([kn[:, n * DN : (n + 1) * DN], rot], axis=1)
                v = vn
                scale = wn ** (-0.5)
            s = lax.dot_general(
                q, k, (((1,), (1,)), ((), ())), preferred_element_type=jnp.float32
            )
            s = jnp.where(allowed, s * scale, masked_score)
            new_max = jnp.maximum(old_max, jnp.max(s, axis=-1, keepdims=True))
            e = jnp.where(allowed, jnp.exp(s - new_max), 0.0)
            factor = jnp.exp(old_max - new_max)
            new_sum = old_sum * factor + jnp.sum(e, axis=-1, keepdims=True)
            pv = jnp.dot(e.astype(jnp.bfloat16), v, preferred_element_type=jnp.float32)
            out.append((new_max, new_sum, old_acc * factor + pv))
        return tuple(out)

    init = tuple(
        (
            jnp.full((rows, 1), masked_score, jnp.float32),
            jnp.zeros((rows, 1), jnp.float32),
            jnp.zeros((rows, w), jnp.float32),
        )
        for w in widths
    )
    final = lax.fori_loop(0, blocks, step, init)
    parts = [final[h][2] / final[h][1] for h in range(heads)]
    for h in range(broad):
        for t in range(o_ref.shape[0]):
            o_ref[t, :, h * DB : (h + 1) * DB] = parts[h][t * share : (t + 1) * share].astype(
                o_ref.dtype
            )
    if narrow:
        column = lax.broadcasted_iota(jnp.int32, parts[broad].shape, 1)
        mixed = parts[broad]
        for n in range(1, narrow):
            mixed = jnp.where(column >= n * DN, parts[broad + n], mixed)
        for t in range(o_ref.shape[0]):
            o_ref[t, :, broad * DB :] = mixed[t * share : (t + 1) * share].astype(o_ref.dtype)


def layer_kernel(
    sp,
    tp,
    mine_ref,
    qb_ref,
    qn_ref,
    resid_ref,
    kb_ref,
    vb_ref,
    kn_ref,
    vn_ref,
    ob_hbm,
    on_hbm,
    post_ref,
    gain_ref,
    last_ref,
    up_hbm,
    down_hbm,
    out_ref,
    lat,
    attn,
    heads,
    ob,
    on,
    up,
    down,
    rows,
    total,
    core_send,
    core_got,
    x_send,
    x_got,
    z_send,
    z_got,
    send_sem,
    recv_sem,
    local_sem,
):
    cols = row_parts
    lines = sp // cols
    s = lax.axis_index("sp")
    t = lax.axis_index("tp")
    z = s // cols
    y = s % cols
    core = t % 2
    ports = t // 2
    t_core = t + 1 - 2 * core
    t_x = (1 - ports) * 2 + core
    t_both = (1 - ports) * 2 + (1 - core)
    s_y = z * cols + 1 - y
    bf16 = jnp.bfloat16
    share = resid_ref.shape[0]
    width = up.shape[2]

    def line(k):
        return (z + k + lines) % lines * cols + y

    def source(k, flipped):
        return (z - k + lines) % lines * cols + ((1 - y) if flipped else y)

    peers = [(line(k), t) for k in range(1, lines)]
    peers += [(s_y, t), (s, t_core), (s, t_x), (s, t_both)]
    barrier = pltpu.get_barrier_semaphore()
    for peer in peers:
        pl.semaphore_signal(
            barrier, inc=1, device_id=peer, device_id_type=pl.DeviceIdType.MESH
        )
    pl.semaphore_wait(barrier, len(peers))

    started = []

    def send(src, dst, peer):
        i = len(started)
        copy = pltpu.make_async_remote_copy(
            src_ref=src,
            dst_ref=dst,
            send_sem=send_sem.at[i],
            recv_sem=recv_sem.at[i],
            device_id=peer,
            device_id_type=pl.DeviceIdType.MESH,
        )
        copy.start()
        started.append(copy)
        return copy

    locals_ = []

    def bring(src, dst):
        copy = pltpu.make_async_copy(src, dst, local_sem.at[len(locals_)])
        copy.start()
        locals_.append(copy)
        return copy

    def cut(ref, k):
        at = pl.multiple_of((z + k) % lines * width, width)
        return ref.at[:, pl.ds(at, width)]

    far = list(range(1, lines))
    lat_z = {k: send(mine_ref, lat.at[s, core], (line(k), t)) for k in far}
    lat_y = {0: send(mine_ref, lat.at[s, core], (s_y, t))}
    lat_c = [send(mine_ref, lat.at[s, core], (s, t_core))]
    up_z = {k: send(cut(up_hbm, k), up.at[s], (line(k), t)) for k in far}
    down_z = {k: send(cut(down_hbm, k), down.at[s], (line(k), t)) for k in far}
    own = [bring(cut(up_hbm, 0), up.at[s]), bring(cut(down_hbm, 0), down.at[s])]
    outs = [bring(ob_hbm, ob), bring(on_hbm, on)]
    lat[s, core] = mine_ref[...]
    order = sorted(far, key=lambda k: min(k, lines - k))
    for k in order:
        lat_z[k].wait_recv()
        held = lat.at[source(k, False), core]
        lat_y[k] = send(held, held, (s_y, t))
        lat_c.append(send(held, held, (s, t_core)))
    for k in [0] + order:
        lat_y[k].wait_recv()
        held = lat.at[source(k, True), core]
        lat_c.append(send(held, held, (s, t_core)))
    up_y = [send(cut(up_hbm, 0), up.at[s], (s_y, t))]
    down_y = [send(cut(down_hbm, 0), down.at[s], (s_y, t))]
    for copy in lat_c:
        copy.wait_recv()

    attend_rows(qb_ref, qn_ref, lat, kb_ref, vb_ref, kn_ref, vn_ref, attn)

    moved = [
        send(attn.at[peer], heads.at[t], (s, peer)) for peer in (t_x, t_both, t_core)
    ]
    heads[t] = attn[t]
    for k in order:
        up_z[k].wait_recv()
        held = up.at[source(k, False)]
        up_y.append(send(held, held, (s_y, t)))
    for copy in outs:
        copy.wait()
    for copy in moved:
        copy.wait_recv()

    broad_width = kb_ref.shape[1]
    narrow_width = kn_ref.shape[1]
    projected = jnp.zeros((share, ob.shape[1]), jnp.float32)
    for i in range(tp):
        projected = projected + jnp.dot(
            heads[i, :, :broad_width],
            ob[i * broad_width : (i + 1) * broad_width],
            preferred_element_type=jnp.float32,
        )
        projected = projected + jnp.dot(
            heads[i, :, broad_width:],
            on[i * narrow_width : (i + 1) * narrow_width],
            preferred_element_type=jnp.float32,
        )
    mixed = (
        resid_ref[...].astype(jnp.float32) + rms_scale(projected, post_ref[...])
    ).astype(bf16)
    rows[0, 0] = rms_scale(mixed.astype(jnp.float32), gain_ref[...]).astype(bf16)

    row_z = {k: send(rows.at[0, 0], rows.at[0, k], (line(k), t)) for k in far}
    row_x = {0: send(rows.at[0, 0], rows.at[1, 0], (s, t_x))}
    row_c = {0: send(rows.at[0, 0], rows.at[2, 0], (s, t_core))}
    row_b = {}
    for k in order:
        down_z[k].wait_recv()
        held = down.at[source(k, False)]
        down_y.append(send(held, held, (s_y, t)))
    row_x[0].wait_recv()
    row_b[0] = send(rows.at[1, 0], rows.at[3, 0], (s, t_core))
    for k in order:
        row_z[k].wait_recv()
        row_x[k] = send(rows.at[0, k], rows.at[1, k], (s, t_x))
        row_c[k] = send(rows.at[0, k], rows.at[2, k], (s, t_core))
    for copy in own:
        copy.wait()
    for copy in up_y + down_y:
        copy.wait_recv()

    deep = sp * up.shape[1]

    def feed(j):
        block = rows[j].reshape(lines * share, rows.shape[3])
        product = jnp.dot(block, up[...].reshape(deep, width), preferred_element_type=jnp.float32)
        hidden = jnp.square(jnp.maximum(product, 0.0)).astype(bf16)
        return lax.dot_general(
            hidden,
            down[...].reshape(deep, width),
            (((1,), (1,)), ((), ())),
            preferred_element_type=jnp.float32,
        )

    total[0] = feed(0)
    for k in [0] + order:
        row_c[k].wait_recv()
    core_send[0] = feed(2).astype(bf16)
    sum_c = [send(core_send.at[0], core_got.at[0], (s, t_core))]
    for k in order:
        row_x[k].wait_recv()
        row_b[k] = send(rows.at[1, k], rows.at[3, k], (s, t_core))
    total[1] = feed(1)
    for k in [0] + order:
        row_b[k].wait_recv()
    core_send[1] = feed(3).astype(bf16)
    sum_c.append(send(core_send.at[1], core_got.at[1], (s, t_core)))
    sum_c[1].wait_recv()
    sum_x = {}
    back = order[::-1] + [0]
    for k in back:
        part = slice(k * share, (k + 1) * share)
        x_send[k] = (total[1, part] + core_got[1, part].astype(jnp.float32)).astype(bf16)
        sum_x[k] = send(x_send.at[k], x_got.at[k], (s, t_x))
    sum_c[0].wait_recv()
    sum_z = []
    for k in back:
        part = slice(k * share, (k + 1) * share)
        sum_x[k].wait_recv()
        piece = (
            total[0, part]
            + core_got[0, part].astype(jnp.float32)
            + x_got[k].astype(jnp.float32)
        )
        if k:
            z_send[k] = piece.astype(bf16)
            sum_z.append(send(z_send.at[k], z_got.at[k], (line(-k), t)))
        else:
            ffn = piece
    for copy in sum_z:
        copy.wait_recv()
    for k in far:
        ffn = ffn + z_got[k].astype(jnp.float32)
    out_ref[...] = (mixed.astype(jnp.float32) + rms_scale(ffn, last_ref[...])).astype(bf16)
    for copy in started:
        copy.wait_send()


def fast_local(
    resid,
    query_broad,
    query_narrow,
    latent,
    key_rope,
    latent_gain,
    key_up_broad,
    value_up_broad,
    key_up_narrow,
    value_up_narrow,
    out_broad,
    out_narrow,
    post_gain,
    ffn_gain,
    up_weight,
    down_weight,
    ffn_out_gain,
):
    sp = lax.axis_size("sp")
    tp = lax.axis_size("tp")
    cols = row_parts
    lines = sp // cols
    s = lax.axis_index("sp")
    z = s // cols
    y = s % cols
    local_rows = resid.shape[0]
    share_rows = local_rows // tp
    query_pos = s * local_rows + jnp.arange(local_rows, dtype=jnp.int32)
    rope_width = key_rope.shape[1]
    bf16 = jnp.bfloat16

    normed_latent = rms_scale(latent.astype(jnp.float32), latent_gain).astype(bf16)
    key_rot = rotate(key_rope.astype(jnp.float32), query_pos).astype(bf16)
    both = jnp.concatenate([normed_latent, key_rot], axis=1)
    core = lax.axis_index("tp") % 2
    half_rows = local_rows // 2
    mine = lax.dynamic_slice_in_dim(both, core * half_rows, half_rows, 0)
    def rotate_queries(queries, head_size):
        parts = queries.reshape(local_rows, -1, head_size + rope_width)
        rotated = rotate(parts[:, :, head_size:].astype(jnp.float32), query_pos).astype(bf16)
        return jnp.concatenate([parts[:, :, :head_size], rotated], axis=-1).reshape(queries.shape)

    broad_width = key_up_broad.shape[1]
    narrow_width = key_up_narrow.shape[1]
    width = broad_width + narrow_width
    deep = resid.shape[1]
    slice_width = up_weight.shape[1] // lines
    own_resid = lax.dynamic_slice_in_dim(resid, lax.axis_index("tp") * share_rows, share_rows, 0)
    vmem = pl.BlockSpec(memory_space=pltpu.VMEM)
    anywhere = pl.BlockSpec(memory_space=pl.ANY)
    return pl.pallas_call(
        functools.partial(layer_kernel, sp, tp),
        out_shape=jax.ShapeDtypeStruct((share_rows, deep), bf16),
        in_specs=[vmem] * 8 + [anywhere] * 2 + [vmem] * 3 + [anywhere] * 2,
        out_specs=vmem,
        scratch_shapes=[
            pltpu.VMEM((sp, 2, half_rows, both.shape[1]), bf16),
            pltpu.VMEM((tp, share_rows, width), bf16),
            pltpu.VMEM((tp, share_rows, width), bf16),
            pltpu.VMEM(out_broad.shape, bf16),
            pltpu.VMEM(out_narrow.shape, bf16),
            pltpu.VMEM((sp, up_weight.shape[0], slice_width), bf16),
            pltpu.VMEM((sp, up_weight.shape[0], slice_width), bf16),
            pltpu.VMEM((tp, lines, share_rows, deep), bf16),
            pltpu.VMEM((2, lines * share_rows, deep), jnp.float32),
            pltpu.VMEM((2, lines * share_rows, deep), bf16),
            pltpu.VMEM((2, lines * share_rows, deep), bf16),
            pltpu.VMEM((lines, share_rows, deep), bf16),
            pltpu.VMEM((lines, share_rows, deep), bf16),
            pltpu.VMEM((lines, share_rows, deep), bf16),
            pltpu.VMEM((lines, share_rows, deep), bf16),
            pltpu.SemaphoreType.DMA((15 * lines + 2,)),
            pltpu.SemaphoreType.DMA((15 * lines + 2,)),
            pltpu.SemaphoreType.DMA((4,)),
        ],
        compiler_params=pltpu.CompilerParams(
            collective_id=0, has_side_effects=True, vmem_limit_bytes=60 * 2**20
        ),
    )(
        mine,
        rotate_queries(query_broad, DB),
        rotate_queries(query_narrow, DN),
        own_resid,
        key_up_broad,
        value_up_broad,
        key_up_narrow,
        value_up_narrow,
        out_broad,
        out_narrow,
        post_gain[None],
        ffn_gain[None],
        ffn_out_gain[None],
        up_weight,
        down_weight,
    )


def solution(mesh):
    in_specs = (
        P("sp", None),
        P("sp", "tp"),
        P("sp", "tp"),
        P("sp", None),
        P("sp", None),
        P(),
        P(None, "tp"),
        P(None, "tp"),
        P(None, "tp"),
        P(None, "tp"),
        P(),
        P(),
        P(),
        P(),
        P("sp", "tp"),
        P("sp", "tp"),
        P(),
    )
    out_specs = P(("sp", "tp"), None)
    sp = mesh.shape["sp"]
    tp = mesh.shape["tp"]

    def whole(*args):
        hidden = args[14].shape[1] // tp
        rows = args[0].shape[0] // sp
        lines = sp // row_parts
        fits = (
            sp % row_parts == 0
            and tp & (tp - 1) == 0
            and tp == 4
            and lines > 1
            and hidden % (lines * lane_tile) == 0
            and rows % (16 * tp) == 0
        )
        body = fast_local if fits else local
        return jax.shard_map(
            body, mesh=mesh, in_specs=in_specs, out_specs=out_specs, check_vma=False
        )(*args)

    return whole
```

```python
import functools
import math

import jax
import jax.numpy as jnp
from jax import lax
from jax.experimental import pallas as pl
from jax.experimental.pallas import tpu as pltpu
from jax.sharding import PartitionSpec as P

DB = 128
DN = 64


norm_eps = 1e-06
rope_base = 500000.0
masked_score = -1e30


def rotate(values, positions):
    full_width = values.shape[-1]
    half_width = full_width // 2
    frequency = rope_base ** (-2.0 * jnp.arange(half_width, dtype=jnp.float32) / full_width)
    angles = positions.astype(jnp.float32)[:, None] * frequency[None, :]
    angle_shape = (angles.shape[0],) + (1,) * (values.ndim - 2) + (half_width,)
    cosine = jnp.cos(angles).reshape(angle_shape)
    sine_part = jnp.sin(angles).reshape(angle_shape)
    leading = values[..., :half_width]
    trailing = values[..., half_width:]
    return jnp.concatenate(
        [leading * cosine - trailing * sine_part, trailing * cosine + leading * sine_part], axis=-1
    )


def rms_scale(values, norm_gain):
    return (
        values * lax.rsqrt(jnp.mean(values * values, axis=-1, keepdims=True) + norm_eps) * norm_gain
    )


def group_update(
    running, nope_query, rope_query, key_rows, key_rot, value_rows, score_scale, allowed
):
    old_max, old_sum, old_acc = running
    scores = jnp.einsum("qhd,khd->hqk", nope_query, key_rows, preferred_element_type=jnp.float32)
    scores = scores + jnp.einsum(
        "qhd,kd->hqk", rope_query, key_rot, preferred_element_type=jnp.float32
    )
    scores = jnp.where(allowed, scores * score_scale, masked_score)
    new_max = jnp.maximum(old_max, jnp.max(scores, axis=-1))
    exponent = jnp.where(allowed, jnp.exp(scores - new_max[:, :, None]), 0.0)
    factor = jnp.exp(old_max - new_max)
    new_sum = old_sum * factor + jnp.sum(exponent, axis=-1)
    weighted = jnp.einsum(
        "hqk,khd->qhd",
        exponent.astype(jnp.bfloat16),
        value_rows,
        preferred_element_type=jnp.float32,
    )
    new_acc = old_acc * jnp.transpose(factor)[:, :, None] + weighted
    return (new_max, new_sum, new_acc)


def local(
    resid,
    query_broad,
    query_narrow,
    latent,
    key_rope,
    latent_gain,
    key_up_broad,
    value_up_broad,
    key_up_narrow,
    value_up_narrow,
    out_broad,
    out_narrow,
    post_gain,
    ffn_gain,
    up_weight,
    down_weight,
    ffn_out_gain,
):
    local_rows = resid.shape[0]
    head_parts = lax.axis_size("tp")
    share_rows = local_rows // head_parts
    row_offset = lax.axis_index("sp") * local_rows
    last_query = row_offset + local_rows - 1
    query_pos = row_offset + jnp.arange(local_rows, dtype=jnp.int32)
    rope_width = key_rope.shape[1]
    broad_count = key_up_broad.shape[1] // DB
    narrow_count = key_up_narrow.shape[1] // DN
    broad_heads = query_broad.reshape(local_rows, broad_count, DB + rope_width)
    broad_nope = broad_heads[:, :, :DB]
    broad_rope = rotate(broad_heads[:, :, DB:].astype(jnp.float32), query_pos).astype(jnp.bfloat16)
    narrow_heads = query_narrow.reshape(local_rows, narrow_count, DN + rope_width)
    narrow_nope = narrow_heads[:, :, :DN]
    narrow_rope = rotate(narrow_heads[:, :, DN:].astype(jnp.float32), query_pos).astype(
        jnp.bfloat16
    )
    broad_scale = (DB + rope_width) ** (-0.5)
    narrow_scale = (DN + rope_width) ** (-0.5)

    def attend(running, latent_rows, rope_rows, first_row):
        key_count = latent_rows.shape[0]
        key_pos = first_row + jnp.arange(key_count, dtype=jnp.int32)
        latent_normed = rms_scale(latent_rows.astype(jnp.float32), latent_gain).astype(jnp.bfloat16)

        def expand(weight, head_size):
            product = jnp.dot(latent_normed, weight, preferred_element_type=jnp.float32)
            return product.astype(jnp.bfloat16).reshape(key_count, -1, head_size)

        key_rot = rotate(rope_rows.astype(jnp.float32), key_pos).astype(jnp.bfloat16)
        allowed = (key_pos[None, :] <= query_pos[:, None])[None]
        broad_state = group_update(
            running[0],
            broad_nope,
            broad_rope,
            expand(key_up_broad, DB),
            key_rot,
            expand(value_up_broad, DB),
            broad_scale,
            allowed,
        )
        narrow_state = group_update(
            running[1],
            narrow_nope,
            narrow_rope,
            expand(key_up_narrow, DN),
            key_rot,
            expand(value_up_narrow, DN),
            narrow_scale,
            allowed,
        )
        return (broad_state, narrow_state)

    def fresh(head_count, head_size):
        return (
            jnp.full((head_count, local_rows), masked_score, jnp.float32),
            jnp.zeros((head_count, local_rows), jnp.float32),
            jnp.zeros((local_rows, head_count, head_size), jnp.float32),
        )

    initial = (fresh(broad_count, DB), fresh(narrow_count, DN))
    latent_piece = lax.all_gather(latent, "sp", axis=0, tiled=True)
    rope_piece = lax.all_gather(key_rope, "sp", axis=0, tiled=True)
    piece_rows = latent_piece.shape[0]
    block_rows = math.gcd(piece_rows, 1024)

    def one_block(block_index, carried):
        begin = block_index * block_rows
        latent_block = lax.dynamic_slice_in_dim(latent_piece, begin, block_rows, 0)
        rope_block = lax.dynamic_slice_in_dim(rope_piece, begin, block_rows, 0)

        def unchanged(kept_state):
            return kept_state

        def updated(kept_state):
            return attend(kept_state, latent_block, rope_block, begin)

        return lax.cond(begin > last_query, unchanged, updated, carried)

    final_state = lax.fori_loop(0, piece_rows // block_rows, one_block, initial)

    def finish(running):
        run_max, run_sum, run_acc = running
        return (
            (run_acc / jnp.transpose(run_sum)[:, :, None])
            .astype(jnp.bfloat16)
            .reshape(local_rows, -1)
        )

    attn_broad = finish(final_state[0])
    attn_narrow = finish(final_state[1])
    rows_broad, rows_narrow = (
        lax.all_to_all(attn_broad, "tp", split_axis=0, concat_axis=1, tiled=True),
        lax.all_to_all(attn_narrow, "tp", split_axis=0, concat_axis=1, tiled=True),
    )
    projected = jnp.dot(rows_broad, out_broad, preferred_element_type=jnp.float32) + jnp.dot(
        rows_narrow, out_narrow, preferred_element_type=jnp.float32
    )
    own_resid = lax.dynamic_slice_in_dim(resid, lax.axis_index("tp") * share_rows, share_rows, 0)
    mixed = (own_resid.astype(jnp.float32) + rms_scale(projected, post_gain)).astype(jnp.bfloat16)
    normed = rms_scale(mixed.astype(jnp.float32), ffn_gain).astype(jnp.bfloat16)
    up_full, down_full = (
        lax.all_gather(up_weight, "sp", axis=0, tiled=True),
        lax.all_gather(down_weight, "sp", axis=0, tiled=True),
    )
    hidden = jnp.square(
        jax.nn.relu(
            jnp.dot(
                lax.all_gather(normed, "tp", axis=0, tiled=True),
                up_full,
                preferred_element_type=jnp.float32,
            )
        )
    ).astype(jnp.bfloat16)
    ffn = lax.psum_scatter(
        lax.dot_general(
            hidden, down_full, (((1,), (1,)), ((), ())), preferred_element_type=jnp.float32
        ).astype(jnp.bfloat16),
        "tp",
        scatter_dimension=0,
        tiled=True,
    ).astype(jnp.float32)
    return (mixed.astype(jnp.float32) + rms_scale(ffn, ffn_out_gain)).astype(jnp.bfloat16)

lane_tile = 128
row_parts = 2


def attend_rows(qb_ref, qn_ref, lat_ref, kb_ref, vb_ref, kn_ref, vn_ref, o_ref):
    rows = qb_ref.shape[0]
    latent_width = kb_ref.shape[0]
    rope = lat_ref.shape[3] - latent_width
    share = o_ref.shape[1]
    block = 2 * rows
    broad = kb_ref.shape[1] // DB
    narrow = kn_ref.shape[1] // DN
    first = lax.axis_index("sp") * rows
    blocks = lax.div(first + rows + block - 1, block)
    query_pos = first + lax.broadcasted_iota(jnp.int32, (rows, block), 0)
    key_iota = lax.broadcasted_iota(jnp.int32, (rows, block), 1)
    wb = DB + rope
    wn = DN + rope
    heads = broad + narrow
    widths = [DB] * broad + [narrow * DN] * narrow

    def step(index, carried):
        start = pl.multiple_of(index * block, block)
        both = lat_ref[pl.ds(2 * index, 2)].reshape(block, latent_width + rope)
        lat = both[:, :latent_width]
        rot = both[:, latent_width:]

        def expand(ref):
            return jnp.dot(lat, ref[...], preferred_element_type=jnp.float32).astype(jnp.bfloat16)

        kb, vb, kn, vn = expand(kb_ref), expand(vb_ref), expand(kn_ref), expand(vn_ref)
        allowed = key_iota + start <= query_pos
        out = []
        for h in range(heads):
            old_max, old_sum, old_acc = carried[h]
            if h < broad:
                q = qb_ref[:, h * wb : (h + 1) * wb]
                k = jnp.concatenate([kb[:, h * DB : (h + 1) * DB], rot], axis=1)
                v = vb[:, h * DB : (h + 1) * DB]
                scale = wb ** (-0.5)
            else:
                n = h - broad
                q = qn_ref[:, n * wn : (n + 1) * wn]
                k = jnp.concatenate([kn[:, n * DN : (n + 1) * DN], rot], axis=1)
                v = vn
                scale = wn ** (-0.5)
            s = lax.dot_general(
                q, k, (((1,), (1,)), ((), ())), preferred_element_type=jnp.float32
            )
            s = jnp.where(allowed, s * scale, masked_score)
            new_max = jnp.maximum(old_max, jnp.max(s, axis=-1, keepdims=True))
            e = jnp.where(allowed, jnp.exp(s - new_max), 0.0)
            factor = jnp.exp(old_max - new_max)
            new_sum = old_sum * factor + jnp.sum(e, axis=-1, keepdims=True)
            pv = jnp.dot(e.astype(jnp.bfloat16), v, preferred_element_type=jnp.float32)
            out.append((new_max, new_sum, old_acc * factor + pv))
        return tuple(out)

    init = tuple(
        (
            jnp.full((rows, 1), masked_score, jnp.float32),
            jnp.zeros((rows, 1), jnp.float32),
            jnp.zeros((rows, w), jnp.float32),
        )
        for w in widths
    )
    final = lax.fori_loop(0, blocks, step, init)
    parts = [final[h][2] / final[h][1] for h in range(heads)]
    for h in range(broad):
        for t in range(o_ref.shape[0]):
            o_ref[t, :, h * DB : (h + 1) * DB] = parts[h][t * share : (t + 1) * share].astype(
                o_ref.dtype
            )
    if narrow:
        column = lax.broadcasted_iota(jnp.int32, parts[broad].shape, 1)
        mixed = parts[broad]
        for n in range(1, narrow):
            mixed = jnp.where(column >= n * DN, parts[broad + n], mixed)
        for t in range(o_ref.shape[0]):
            o_ref[t, :, broad * DB :] = mixed[t * share : (t + 1) * share].astype(o_ref.dtype)


def layer_kernel(
    sp,
    tp,
    latent_ref,
    key_rope_ref,
    table_ref,
    latent_gain_ref,
    qb_in,
    qn_in,
    resid_ref,
    kb_ref,
    vb_ref,
    kn_ref,
    vn_ref,
    ob_hbm,
    on_hbm,
    post_ref,
    gain_ref,
    last_ref,
    up_hbm,
    down_hbm,
    out_ref,
    mine_ref,
    qb_ref,
    qn_ref,
    lat,
    attn,
    heads,
    ob,
    on,
    up,
    down,
    rows,
    total,
    core_send,
    core_got,
    x_send,
    x_got,
    z_send,
    z_got,
    send_sem,
    recv_sem,
    local_sem,
):
    cols = row_parts
    lines = sp // cols
    s = lax.axis_index("sp")
    t = lax.axis_index("tp")
    z = s // cols
    y = s % cols
    core = t % 2
    ports = t // 2
    t_core = t + 1 - 2 * core
    t_x = (1 - ports) * 2 + core
    t_both = (1 - ports) * 2 + (1 - core)
    s_y = z * cols + 1 - y
    bf16 = jnp.bfloat16
    share = resid_ref.shape[0] // tp
    width = up.shape[2]

    def line(k):
        return (z + k + lines) % lines * cols + y

    def source(k, flipped):
        return (z - k + lines) % lines * cols + ((1 - y) if flipped else y)

    peers = [(line(k), t) for k in range(1, lines)]
    peers += [(s_y, t), (s, t_core), (s, t_x), (s, t_both)]
    barrier = pltpu.get_barrier_semaphore()
    for peer in peers:
        pl.semaphore_signal(
            barrier, inc=1, device_id=peer, device_id_type=pl.DeviceIdType.MESH
        )

    rope = key_rope_ref.shape[1]
    half_rope = rope // 2

    def turn(values, table):
        values = values.astype(jnp.float32)
        swapped = jnp.concatenate([values[:, half_rope:], values[:, :half_rope]], axis=1)
        return (values * table[:, :rope] + swapped * table[:, rope:]).astype(bf16)

    latent_width = latent_ref.shape[1]
    half = mine_ref.shape[0]
    mine_rows = pl.ds(pl.multiple_of(core * half, 16), half)
    mine_ref[:, :latent_width] = rms_scale(
        latent_ref[mine_rows, :].astype(jnp.float32), latent_gain_ref[...]
    ).astype(bf16)
    mine_ref[:, latent_width:] = turn(key_rope_ref[mine_rows, :], table_ref[mine_rows, :])
    pl.semaphore_wait(barrier, len(peers))

    started = []

    def send(src, dst, peer):
        i = len(started)
        copy = pltpu.make_async_remote_copy(
            src_ref=src,
            dst_ref=dst,
            send_sem=send_sem.at[i],
            recv_sem=recv_sem.at[i],
            device_id=peer,
            device_id_type=pl.DeviceIdType.MESH,
        )
        copy.start()
        started.append(copy)
        return copy

    locals_ = []

    def bring(src, dst):
        copy = pltpu.make_async_copy(src, dst, local_sem.at[len(locals_)])
        copy.start()
        locals_.append(copy)
        return copy

    def cut(ref, k):
        at = pl.multiple_of((z + k) % lines * width, width)
        return ref.at[:, pl.ds(at, width)]

    far = list(range(1, lines))
    lat_z = {k: send(mine_ref, lat.at[s, core], (line(k), t)) for k in far}
    lat_y = {0: send(mine_ref, lat.at[s, core], (s_y, t))}
    lat_c = [send(mine_ref, lat.at[s, core], (s, t_core))]
    up_z = {k: send(cut(up_hbm, k), up.at[s], (line(k), t)) for k in far}
    down_z = {k: send(cut(down_hbm, k), down.at[s], (line(k), t)) for k in far}
    own = [bring(cut(up_hbm, 0), up.at[s]), bring(cut(down_hbm, 0), down.at[s])]
    outs = [bring(ob_hbm, ob), bring(on_hbm, on)]
    lat[s, core] = mine_ref[...]
    for queries, turned, size in ((qb_in, qb_ref, DB), (qn_in, qn_ref, DN)):
        step = size + rope
        for h in range(queries.shape[1] // step):
            middle = h * step + size
            turned[:, h * step : middle] = queries[:, h * step : middle]
            turned[:, middle : middle + rope] = turn(
                queries[:, middle : middle + rope], table_ref[...]
            )
    order = sorted(far, key=lambda k: min(k, lines - k))
    for k in order:
        lat_z[k].wait_recv()
        held = lat.at[source(k, False), core]
        lat_y[k] = send(held, held, (s_y, t))
        lat_c.append(send(held, held, (s, t_core)))
    for k in [0] + order:
        lat_y[k].wait_recv()
        held = lat.at[source(k, True), core]
        lat_c.append(send(held, held, (s, t_core)))
    up_y = [send(cut(up_hbm, 0), up.at[s], (s_y, t))]
    down_y = [send(cut(down_hbm, 0), down.at[s], (s_y, t))]
    for copy in lat_c:
        copy.wait_recv()

    attend_rows(qb_ref, qn_ref, lat, kb_ref, vb_ref, kn_ref, vn_ref, attn)

    moved = [
        send(attn.at[peer], heads.at[t], (s, peer)) for peer in (t_x, t_both, t_core)
    ]
    heads[t] = attn[t]
    for k in order:
        up_z[k].wait_recv()
        held = up.at[source(k, False)]
        up_y.append(send(held, held, (s_y, t)))
    for copy in outs:
        copy.wait()
    for copy in moved:
        copy.wait_recv()

    broad_width = kb_ref.shape[1]
    narrow_width = kn_ref.shape[1]
    projected = jnp.zeros((share, ob.shape[1]), jnp.float32)
    for i in range(tp):
        projected = projected + jnp.dot(
            heads[i, :, :broad_width],
            ob[i * broad_width : (i + 1) * broad_width],
            preferred_element_type=jnp.float32,
        )
        projected = projected + jnp.dot(
            heads[i, :, broad_width:],
            on[i * narrow_width : (i + 1) * narrow_width],
            preferred_element_type=jnp.float32,
        )
    mixed = (
        resid_ref[pl.ds(pl.multiple_of(t * share, 16), share), :].astype(jnp.float32)
        + rms_scale(projected, post_ref[...])
    ).astype(bf16)
    rows[0, 0] = rms_scale(mixed.astype(jnp.float32), gain_ref[...]).astype(bf16)

    row_z = {k: send(rows.at[0, 0], rows.at[0, k], (line(k), t)) for k in far}
    row_x = {0: send(rows.at[0, 0], rows.at[1, 0], (s, t_x))}
    row_c = {0: send(rows.at[0, 0], rows.at[2, 0], (s, t_core))}
    row_b = {}
    for k in order:
        down_z[k].wait_recv()
        held = down.at[source(k, False)]
        down_y.append(send(held, held, (s_y, t)))
    row_x[0].wait_recv()
    row_b[0] = send(rows.at[1, 0], rows.at[3, 0], (s, t_core))
    for k in order:
        row_z[k].wait_recv()
        row_x[k] = send(rows.at[0, k], rows.at[1, k], (s, t_x))
        row_c[k] = send(rows.at[0, k], rows.at[2, k], (s, t_core))
    for copy in own:
        copy.wait()
    for copy in up_y + down_y:
        copy.wait_recv()

    deep = sp * up.shape[1]

    def feed(j):
        block = rows[j].reshape(lines * share, rows.shape[3])
        product = jnp.dot(block, up[...].reshape(deep, width), preferred_element_type=jnp.float32)
        hidden = jnp.square(jnp.maximum(product, 0.0)).astype(bf16)
        return lax.dot_general(
            hidden,
            down[...].reshape(deep, width),
            (((1,), (1,)), ((), ())),
            preferred_element_type=jnp.float32,
        )

    total[0] = feed(0)
    for k in [0] + order:
        row_c[k].wait_recv()
    core_send[0] = feed(2).astype(bf16)
    sum_c = [send(core_send.at[0], core_got.at[0], (s, t_core))]
    for k in order:
        row_x[k].wait_recv()
        row_b[k] = send(rows.at[1, k], rows.at[3, k], (s, t_core))
    total[1] = feed(1)
    for k in [0] + order:
        row_b[k].wait_recv()
    core_send[1] = feed(3).astype(bf16)
    sum_c.append(send(core_send.at[1], core_got.at[1], (s, t_core)))
    sum_c[1].wait_recv()
    sum_x = {}
    back = order[::-1] + [0]
    for k in back:
        part = slice(k * share, (k + 1) * share)
        x_send[k] = (total[1, part] + core_got[1, part].astype(jnp.float32)).astype(bf16)
        sum_x[k] = send(x_send.at[k], x_got.at[k], (s, t_x))
    sum_c[0].wait_recv()
    sum_z = []
    for k in back:
        part = slice(k * share, (k + 1) * share)
        sum_x[k].wait_recv()
        piece = (
            total[0, part]
            + core_got[0, part].astype(jnp.float32)
            + x_got[k].astype(jnp.float32)
        )
        if k:
            z_send[k] = piece.astype(bf16)
            sum_z.append(send(z_send.at[k], z_got.at[k], (line(-k), t)))
        else:
            ffn = piece
    for copy in sum_z:
        copy.wait_recv()
    for k in far:
        ffn = ffn + z_got[k].astype(jnp.float32)
    out_ref[...] = (mixed.astype(jnp.float32) + rms_scale(ffn, last_ref[...])).astype(bf16)
    for copy in started:
        copy.wait_send()


def fast_local(
    resid,
    query_broad,
    query_narrow,
    latent,
    key_rope,
    latent_gain,
    key_up_broad,
    value_up_broad,
    key_up_narrow,
    value_up_narrow,
    out_broad,
    out_narrow,
    post_gain,
    ffn_gain,
    up_weight,
    down_weight,
    ffn_out_gain,
):
    sp = lax.axis_size("sp")
    tp = lax.axis_size("tp")
    cols = row_parts
    lines = sp // cols
    s = lax.axis_index("sp")
    z = s // cols
    y = s % cols
    local_rows = resid.shape[0]
    share_rows = local_rows // tp
    query_pos = s * local_rows + jnp.arange(local_rows, dtype=jnp.int32)
    rope_width = key_rope.shape[1]
    bf16 = jnp.bfloat16

    frequency = rope_base ** (-2.0 * jnp.arange(rope_width // 2, dtype=jnp.float32) / rope_width)
    angles = query_pos.astype(jnp.float32)[:, None] * frequency[None, :]
    cosine, sine = jnp.cos(angles), jnp.sin(angles)
    table = jnp.concatenate([cosine, cosine, -sine, sine], axis=1)
    half_rows = local_rows // 2
    both_width = latent.shape[1] + rope_width
    broad_width = key_up_broad.shape[1]
    narrow_width = key_up_narrow.shape[1]
    width = broad_width + narrow_width
    deep = resid.shape[1]
    slice_width = up_weight.shape[1] // lines
    vmem = pl.BlockSpec(memory_space=pltpu.VMEM)
    anywhere = pl.BlockSpec(memory_space=pl.ANY)
    return pl.pallas_call(
        functools.partial(layer_kernel, sp, tp),
        out_shape=jax.ShapeDtypeStruct((share_rows, deep), bf16),
        in_specs=[vmem] * 11 + [anywhere] * 2 + [vmem] * 3 + [anywhere] * 2,
        out_specs=vmem,
        scratch_shapes=[
            pltpu.VMEM((half_rows, both_width), bf16),
            pltpu.VMEM(query_broad.shape, bf16),
            pltpu.VMEM(query_narrow.shape, bf16),
            pltpu.VMEM((sp, 2, half_rows, both_width), bf16),
            pltpu.VMEM((tp, share_rows, width), bf16),
            pltpu.VMEM((tp, share_rows, width), bf16),
            pltpu.VMEM(out_broad.shape, bf16),
            pltpu.VMEM(out_narrow.shape, bf16),
            pltpu.VMEM((sp, up_weight.shape[0], slice_width), bf16),
            pltpu.VMEM((sp, up_weight.shape[0], slice_width), bf16),
            pltpu.VMEM((tp, lines, share_rows, deep), bf16),
            pltpu.VMEM((2, lines * share_rows, deep), jnp.float32),
            pltpu.VMEM((2, lines * share_rows, deep), bf16),
            pltpu.VMEM((2, lines * share_rows, deep), bf16),
            pltpu.VMEM((lines, share_rows, deep), bf16),
            pltpu.VMEM((lines, share_rows, deep), bf16),
            pltpu.VMEM((lines, share_rows, deep), bf16),
            pltpu.VMEM((lines, share_rows, deep), bf16),
            pltpu.SemaphoreType.DMA((15 * lines + 2,)),
            pltpu.SemaphoreType.DMA((15 * lines + 2,)),
            pltpu.SemaphoreType.DMA((4,)),
        ],
        compiler_params=pltpu.CompilerParams(
            collective_id=0, has_side_effects=True, vmem_limit_bytes=60 * 2**20
        ),
    )(
        latent,
        key_rope,
        table,
        latent_gain[None],
        query_broad,
        query_narrow,
        resid,
        key_up_broad,
        value_up_broad,
        key_up_narrow,
        value_up_narrow,
        out_broad,
        out_narrow,
        post_gain[None],
        ffn_gain[None],
        ffn_out_gain[None],
        up_weight,
        down_weight,
    )


def solution(mesh):
    in_specs = (
        P("sp", None),
        P("sp", "tp"),
        P("sp", "tp"),
        P("sp", None),
        P("sp", None),
        P(),
        P(None, "tp"),
        P(None, "tp"),
        P(None, "tp"),
        P(None, "tp"),
        P(),
        P(),
        P(),
        P(),
        P("sp", "tp"),
        P("sp", "tp"),
        P(),
    )
    out_specs = P(("sp", "tp"), None)
    sp = mesh.shape["sp"]
    tp = mesh.shape["tp"]

    def whole(*args):
        hidden = args[14].shape[1] // tp
        rows = args[0].shape[0] // sp
        lines = sp // row_parts
        fits = (
            sp % row_parts == 0
            and tp & (tp - 1) == 0
            and tp == 4
            and lines > 1
            and hidden % (lines * lane_tile) == 0
            and rows % (16 * tp) == 0
        )
        body = fast_local if fits else local
        return jax.shard_map(
            body, mesh=mesh, in_specs=in_specs, out_specs=out_specs, check_vma=False
        )(*args)

    return whole
```
